256 devices in a mesh: grp: 2 (over y), ra: 16 (over z), cb: 8 (over x, core).
Axes of the slice: x: 4, y: 2, z: 16, core: 2. Of those that a mesh axis runs over, the one named last changes fastest.
The devices are a block of a 4x16x16 slice.
Arguments:
- tokens: bfloat16 [1024, 4096], P('grp', 'ra'), parts along dimension 0, may hold values from -14 to 14
- pre_gain: bfloat16 [2, 4096], P(None, 'ra'), may hold values from 0.099609375 to 1.8984375
- post_gain: bfloat16 [2, 4096], P(None, 'ra'), may hold values from 0.099609375 to 1.8984375
- gate_weight: bfloat16 [2, 4096, 11008], P(None, 'ra', 'cb'), may hold values from -0.09375 to 0.09375
- up_weight: bfloat16 [2, 4096, 11008], P(None, 'ra', 'cb'), may hold values from -0.09375 to 0.09375
- gate_taps: bfloat16 [2, 3, 11008], P(None, None, 'cb'), may hold values from -3 to 3
- up_taps: bfloat16 [2, 3, 11008], P(None, None, 'cb'), may hold values from -3 to 3
- gate_bias: bfloat16 [2, 11008], P(None, 'cb'), may hold values from -3 to 3
- up_bias: bfloat16 [2, 11008], P(None, 'cb'), may hold values from -3 to 3
- down_weight: bfloat16 [2, 11008, 4096], P(None, 'cb', 'ra'), may hold values from -0.07624929 to 0.07624929
Outputs:
- layer_out: bfloat16 [1024, 4096], P('grp', 'ra'), parts along dimension 0
The draws below stay inside these ranges and needn't reach their ends.
There are 2 independent parts, one for each index of `grp`. The reference program is written for one: setup_inputs(seed, part) draws one part's arguments, and reference() takes and returns one part's arrays. A program takes and returns all parts, laid end to end along the dimension named above; an argument that names none is the same for every part. Nothing has to cross between parts.
All inputs are finite; a program needn't handle non-finite values.
Results may differ from the reference program's by a relative error of at most 0.024.
Values may be sent and summed in bfloat16 or wider, within the bound.
No kernel may reach another device: no remote copies, remote signals or barrier semaphores. Data moves between devices by JAX's collectives and lax.ppermute only.
A program may use at most 64 MiB of HBM per device.

```python
import jax
import jax.numpy as jnp
from jax import lax

D = 4096
FF = 11008
TAPS = 3
LAYERS = 2
SEQS = 2
TOKENS = 512
HID_BLOCK = 1376
N_CB = 8


def draw_tokens(key, part):
    key_rows, key_cols, key_vals = jax.random.split(jax.random.fold_in(key, 11), 3)
    position = jnp.arange(D, dtype=jnp.float32)[None, :] / D
    row_log = jax.random.uniform(key_rows, (TOKENS, 1), jnp.float32, -0.5, 0.5) * jnp.log(10.0)
    col_log = (0.5 * position + 0.5 * jax.random.uniform(key_cols, (1, D), jnp.float32) - 0.5) * jnp.log(10.0)
    entries = jnp.clip(jax.random.normal(key_vals, (TOKENS, D), jnp.float32), -4.0, 4.0)
    return (entries * jnp.exp(row_log) * jnp.exp(col_log) / 3.0).astype(jnp.bfloat16)


def draw_down_weight(key, part):
    key_cols, key_vals = jax.random.split(jax.random.fold_in(key, 23), 2)
    position = jnp.arange(D, dtype=jnp.float32)[None, None, :] / D
    spread = jax.random.uniform(key_cols, (LAYERS, 1, D), jnp.float32)
    col_log = (0.5 * position + 0.5 * spread - 0.5) * jnp.log(10.0)
    entries = jnp.clip(jax.random.normal(key_vals, (LAYERS, FF, D), jnp.float32), -2.5, 2.5)
    return (entries * jnp.exp(col_log) / jnp.sqrt(jnp.float32(FF))).astype(jnp.bfloat16)


def level_of(rng, extent, cuts, least, top_value):
    level, own = 1.0, jax.random.fold_in(rng, 6)
    for axis_at, parts in cuts:
        steps = jnp.exp(jax.random.uniform(jax.random.fold_in(own, axis_at), (parts,), jnp.float32, least / len(cuts), top_value / len(cuts)))
        level = level * jnp.repeat(steps, extent[axis_at] // parts).reshape([-1 if axis == axis_at else 1 for axis in range(len(extent))])
    return level


def bell_draw(stream_key, extent, scale, bound, shards=(), kind=jnp.bfloat16):
    values = jax.random.normal(stream_key, extent, jnp.float32) * scale
    if len(shards) > 0:
        values = level_of(stream_key, extent, shards, -0.22, 0.18) * values
    return jnp.clip(values, min=-bound, max=bound).astype(kind)


def setup_inputs(seed: int = 0, part: int = 0) -> dict:
    key_of = jax.random.split(jax.random.key(seed), 11)
    part_splits = jax.random.split(jax.random.fold_in(key_of[10], part), 11)
    tokens = draw_tokens(jax.random.fold_in(jax.random.fold_in(key_of[10], part), 71), part)
    pre_gain = jnp.clip(1.0 + 0.18 * jax.random.normal(key_of[1], (LAYERS, D), jnp.float32), 0.099609375, 1.8984375).astype(jnp.bfloat16)
    post_gain = jnp.clip(1.0 + 0.18 * jax.random.normal(key_of[2], (LAYERS, D), jnp.float32), 0.099609375, 1.8984375).astype(jnp.bfloat16)
    gate_weight = bell_draw(key_of[3], (LAYERS, D, FF), D ** -0.5, 0.09375, ((1, 16), (2, 8)))
    up_weight = bell_draw(key_of[4], (LAYERS, D, FF), D ** -0.5, 0.09375, ((1, 16), (2, 8)))
    gate_taps = bell_draw(key_of[5], (LAYERS, TAPS, FF), 0.577, 3.0, ((2, 8),))
    up_taps = bell_draw(key_of[6], (LAYERS, TAPS, FF), 0.577, 3.0, ((2, 8),))
    gate_bias = bell_draw(key_of[7], (LAYERS, FF), 0.5, 3.0, ((1, 8),))
    up_bias = bell_draw(key_of[8], (LAYERS, FF), 0.5, 3.0, ((1, 8),))
    down_weight = draw_down_weight(jax.random.fold_in(key_of[10], 71), part)
    return dict(tokens=tokens, pre_gain=pre_gain, post_gain=post_gain, gate_weight=gate_weight, up_weight=up_weight, gate_taps=gate_taps, up_taps=up_taps, gate_bias=gate_bias, up_bias=up_bias, down_weight=down_weight)


epsilon = 1e-06
residual_scale = 0.5

def shift_rows(values, delay_by, sequences):
    total_rows, columns = values.shape
    per_sequence = total_rows // sequences
    grouped = values.reshape(sequences, per_sequence, columns)
    moved = jnp.pad(grouped, ((0, 0), (delay_by, 0), (0, 0)))[:, :per_sequence]
    return moved.reshape(total_rows, columns)

def causal_conv(values, tap_weights, sequences):
    tap_count = tap_weights.shape[0]
    result = tap_weights[tap_count - 1] * values
    for offset in range(1, tap_count):
        result = result + tap_weights[tap_count - 1 - offset] * shift_rows(values, offset, sequences)
    return result

def reference(tokens, pre_gain, post_gain, gate_weight, up_weight, gate_taps, up_taps, gate_bias, up_bias, down_weight):
    state = tokens
    for which_layer in range(LAYERS):
        widened = state.astype(jnp.float32)
        pre_scale = lax.rsqrt(lax.optimization_barrier(jnp.sum(widened * widened, axis=1, keepdims=True)) / D + epsilon)
        normed = (widened * pre_gain[which_layer].astype(jnp.float32)).astype(jnp.bfloat16)
        gate_lin = jnp.dot(normed, gate_weight[which_layer], preferred_element_type=jnp.float32) * pre_scale
        up_lin = jnp.dot(normed, up_weight[which_layer], preferred_element_type=jnp.float32) * pre_scale
        gate_conv = causal_conv(gate_lin, gate_taps[which_layer].astype(jnp.float32), SEQS) + gate_bias[which_layer].astype(jnp.float32)
        up_conv = causal_conv(up_lin, up_taps[which_layer].astype(jnp.float32), SEQS) + up_bias[which_layer].astype(jnp.float32)
        hidden = (jax.nn.gelu(gate_conv, approximate=True) * up_conv).astype(jnp.bfloat16)
        blocks = hidden.reshape(TOKENS, N_CB, HID_BLOCK).astype(jnp.float32)
        weights = down_weight[which_layer].reshape(N_CB, HID_BLOCK, D).astype(jnp.float32)
        partials = jnp.einsum('tkf,kfd->ktd', blocks, weights).astype(jnp.bfloat16)
        branch = lax.optimization_barrier(jnp.sum(partials.astype(jnp.float32), axis=0))
        post_scale = lax.rsqrt(lax.optimization_barrier(jnp.sum(branch * branch, axis=1, keepdims=True)) / D + epsilon)
        state = (residual_scale * widened + branch * post_scale * post_gain[which_layer].astype(jnp.float32)).astype(jnp.bfloat16)
    return state
```

```python
import jax
import jax.numpy as jnp
from jax import lax
from jax.sharding import PartitionSpec as P

LEN = 256
LANES = 128
CORES = 2
EPS = 1e-06
RESIDUAL = 0.5
FAR = 1

f32, bf16 = jnp.float32, jnp.bfloat16


def along_ra(x, by):
    n = lax.axis_size("ra")
    return lax.ppermute(x, "ra", [(i, (i + by) % n) for i in range(n)])


def along_chips(x, by):
    n = lax.axis_size("cb")
    return lax.ppermute(x, "cb", [(i, (i + CORES * by) % n) for i in range(n)])


def other_core(x):
    n = lax.axis_size("cb")
    return lax.ppermute(x, "cb", [(i, i ^ 1) for i in range(n)])


def rolled(x, by, unit):
    n = x.shape[0]
    return lax.dynamic_slice_in_dim(jnp.concatenate([x, x], axis=0), by * unit, n, 0)


def ring_sum(part, rim):
    n = len(part)
    half = n // 2
    down, up = part[half], part[half - 1]
    for s in range(half - 1):
        got = along_ra(down, -1)
        down = (got.astype(f32) + part[half + 1 + s].astype(f32)).astype(bf16)
        got = along_ra(up, 1)
        if s < half - 2:
            up = (got.astype(f32) + part[half - 2 - s].astype(f32)).astype(bf16)
        else:
            up = got.astype(f32) + part[0].astype(f32)
    got = along_ra(down, -1)
    before = along_ra(up[-rim:], 1) + down[-rim:].astype(f32)
    return got.astype(f32) + up, before


def ring_apply(own, apply):
    n = lax.axis_size("ra")
    half = n // 2
    far = half // 2 + FAR
    out = [None] * n
    out[0] = apply(own)
    held = {(sign, first): own for sign in (1, -1) for first in (1, far)}
    for k in range(max(far - 1, half - far + 1)):
        for sign in (1, -1):
            for first, last in ((far, half if sign > 0 else half - 1), (1, far - 1)):
                at = first + k
                if at <= last:
                    moved = along_ra(held[sign, first], -sign * (first if k == 0 else 1))
                    held[sign, first] = moved
                    out[sign * at % n] = apply(moved)
    return jnp.concatenate(out, axis=0)


def total_along_ra(x):
    n = lax.axis_size("ra")
    copies = jnp.broadcast_to(x, (n, 1, x.shape[0]))
    return jnp.sum(lax.all_to_all(copies, "ra", split_axis=0, concat_axis=0, tiled=True), axis=(0, 1))


def conv(values, before, taps, positions):
    n, rows = taps.shape[0], values.shape[0]
    extended = jnp.concatenate([before, values], axis=0)
    result = taps[n - 1] * values
    for k in range(1, n):
        moved = extended[n - 1 - k : n - 1 - k + rows]
        result = result + taps[n - 1 - k] * jnp.where(positions >= k, moved, f32(0.0))
    return result


def local(
    tokens, pre_gain, post_gain, gate_weight, up_weight, gate_taps, up_taps, gate_bias, up_bias, down_weight
):
    n_ra = lax.axis_size("ra")
    ra, core = lax.axis_index("ra"), lax.axis_index("cb") % CORES
    layers, width = pre_gain.shape
    rows = tokens.shape[0]
    model = width * n_ra
    chunk, share = rows // n_ra, rows // CORES
    hid = gate_weight.shape[2]
    pad = -hid % LANES
    per = n_ra // CORES
    rim = gate_taps.shape[1] - 1
    state = rolled(tokens, core, share)
    for l in range(layers):
        widened = state.astype(f32)
        squares = jnp.sum(widened * widened, axis=1, keepdims=True)
        normed = (widened * pre_gain[l].astype(f32)).astype(bf16)
        weights = jnp.concatenate(
            [jnp.pad(w[l], ((0, 0), (0, pad))) for w in (gate_weight, up_weight)], axis=1
        )
        high = squares.astype(bf16).astype(f32)
        lane = lax.broadcasted_iota(jnp.int32, (1, 2 * (hid + pad)), 1) - hid
        to_own = (ra + per * core) % n_ra
        normed = rolled(normed, to_own, chunk)
        high, low = rolled(high, to_own, chunk), rolled(squares - high, to_own, chunk)

        def share_of(a, b):
            at = slice(a * chunk, b * chunk)
            extra = jnp.where(lane == ra, high[at], jnp.where(lane == n_ra + ra, low[at], f32(0.0)))
            out = (jnp.dot(normed[at], weights, preferred_element_type=f32) + extra).astype(bf16)
            return [out[k * chunk : (k + 1) * chunk] for k in range(b - a)]

        half = n_ra // 2
        middle = share_of(half - 2, half + 2)
        part = share_of(0, half - 2) + middle + share_of(half + 2, n_ra)
        summed, before = ring_sum(part, rim)

        def scaled(x):
            total = jnp.sum(x[:, hid : hid + 2 * n_ra], axis=1, keepdims=True)
            return x * lax.rsqrt(total / model + EPS)

        lin, before = scaled(summed), scaled(before)
        positions = ((ra * chunk + jnp.arange(chunk, dtype=jnp.int32)) % LEN)[:, None]
        gate, up = (
            conv(lin[:, a : a + hid], before[:, a : a + hid], t[l].astype(f32), positions) + b[l].astype(f32)
            for a, t, b in ((0, gate_taps, gate_bias), (hid + pad, up_taps, up_bias))
        )
        hidden = (jax.nn.gelu(gate, approximate=True) * up).astype(bf16)
        down_rows = down_weight[l]
        partial = ring_apply(hidden, lambda h: jnp.dot(h, down_rows, preferred_element_type=f32).astype(bf16))
        partial = rolled(partial, (n_ra - ra + per * core) % n_ra, chunk)
        pair = (partial[:share].astype(f32) + other_core(partial[share:]).astype(f32)).astype(bf16)
        branch = pair.astype(f32)
        for k in range(1, lax.axis_size("cb") // CORES):
            branch = branch + along_chips(pair, k).astype(f32)
        post_scale = lax.rsqrt(total_along_ra(jnp.sum(branch * branch, axis=1)) / model + EPS)[:, None]
        own = (RESIDUAL * widened[:share] + branch * post_scale * post_gain[l].astype(f32)).astype(bf16)
        state = jnp.concatenate([own, other_core(own)], axis=0)
    return rolled(state, core, share)


def solution(mesh):
    in_specs = (
        P("grp", "ra"),
        P(None, "ra"),
        P(None, "ra"),
        P(None, "ra", "cb"),
        P(None, "ra", "cb"),
        P(None, None, "cb"),
        P(None, None, "cb"),
        P(None, "cb"),
        P(None, "cb"),
        P(None, "cb", "ra"),
    )
    return jax.shard_map(local, mesh=mesh, in_specs=in_specs, out_specs=P("grp", "ra"), check_vma=False)
```

```python
import jax
import jax.numpy as jnp
from jax import lax
from jax.sharding import PartitionSpec as P

LEN = 256
LANES = 128
SUBLANES = 8
CORES = 2
EPS = 1e-06
RESIDUAL = 0.5

f32, bf16 = jnp.float32, jnp.bfloat16


def along_ra(x, by):
    n = lax.axis_size("ra")
    return lax.ppermute(x, "ra", [(i, (i + by) % n) for i in range(n)])


def along_chips(x, by):
    n = lax.axis_size("cb")
    return lax.ppermute(x, "cb", [(i, (i + CORES * by) % n) for i in range(n)])


def other_core(x):
    n = lax.axis_size("cb")
    return lax.ppermute(x, "cb", [(i, i ^ 1) for i in range(n)])


def rolled(x, by, unit):
    n = x.shape[0]
    return lax.dynamic_slice_in_dim(jnp.concatenate([x, x], axis=0), by * unit, n, 0)


def ring_sum(part, rim):
    n = len(part)
    half = n // 2
    down, up = part[half], part[half - 1]
    for s in range(half - 1):
        got = along_ra(down, -1)
        down = (got.astype(f32) + part[half + 1 + s].astype(f32)).astype(bf16)
        got = along_ra(up, 1)
        if s < half - 2:
            up = (got.astype(f32) + part[half - 2 - s].astype(f32)).astype(bf16)
        else:
            up = lax.optimization_barrier(got.astype(f32) + part[0].astype(f32))
    before = along_ra(up[-SUBLANES:].astype(bf16), 1)
    got = along_ra(down, -1)
    before = (before.astype(f32) + down[-SUBLANES:].astype(f32))[-rim:]
    return got.astype(f32) + up, before


def ring_apply(own, apply):
    n = lax.axis_size("ra")
    half, rows = n // 2, own.shape[0]
    far = half // 2 + 1
    out = {0: apply(own)}
    held = {}
    for k in range(far - 1):
        fresh = []
        for sign in (1, -1):
            ends = [1 + k] + ([far + k] if far + k <= (half if sign > 0 else half - 1) else [])
            if k == 0:
                held[sign] = jnp.concatenate([along_ra(own, -sign * e) for e in ends], axis=0)
            else:
                held[sign] = along_ra(held[sign][: len(ends) * rows], -sign)
            fresh += [sign * e % n for e in ends]
        both = apply(jnp.concatenate([held[1], held[-1]], axis=0))
        for i, at in enumerate(fresh):
            out[at] = both[i * rows : (i + 1) * rows]
    return jnp.concatenate([out[at] for at in range(n)], axis=0)


def total_along_ra(x):
    n = lax.axis_size("ra")
    copies = jnp.broadcast_to(x, (n, 1, x.shape[0]))
    return jnp.sum(lax.all_to_all(copies, "ra", split_axis=0, concat_axis=0, tiled=True), axis=(0, 1))


def total_of(values):
    while len(values) > 1:
        half = len(values) // 2
        values = [values[k] + values[k + half] for k in range(half)]
    return values[0]


def conv(values, before, taps, positions):
    n, rows = taps.shape[0], values.shape[0]
    extended = jnp.concatenate([before, values], axis=0)
    result = taps[n - 1] * values
    for k in range(1, n):
        moved = extended[n - 1 - k : n - 1 - k + rows]
        result = result + taps[n - 1 - k] * jnp.where(positions >= k, moved, f32(0.0))
    return result


def local(
    tokens, pre_gain, post_gain, gate_weight, up_weight, gate_taps, up_taps, gate_bias, up_bias, down_weight
):
    n_ra = lax.axis_size("ra")
    ra, core = lax.axis_index("ra"), lax.axis_index("cb") % CORES
    layers, width = pre_gain.shape
    rows = tokens.shape[0]
    model = width * n_ra
    chunk, share = rows // n_ra, rows // CORES
    hid = gate_weight.shape[2]
    pad = -hid % LANES
    per = n_ra // CORES
    rim = gate_taps.shape[1] - 1
    state = rolled(tokens, core, share)
    for l in range(layers):
        widened = state.astype(f32)
        squares = jnp.sum(widened * widened, axis=1, keepdims=True)
        normed = (widened * pre_gain[l].astype(f32)).astype(bf16)
        weights = jnp.concatenate(
            [jnp.pad(w[l], ((0, 0), (0, pad))) for w in (gate_weight, up_weight)], axis=1
        )
        high = squares.astype(bf16).astype(f32)
        lane = lax.broadcasted_iota(jnp.int32, (1, 2 * (hid + pad)), 1) - hid
        to_own = (ra + per * core) % n_ra
        normed = rolled(normed, to_own, chunk)
        high, low = rolled(high, to_own, chunk), rolled(squares - high, to_own, chunk)

        def share_of(a, b):
            at = slice(a * chunk, b * chunk)
            extra = jnp.where(lane == ra, high[at], jnp.where(lane == n_ra + ra, low[at], f32(0.0)))
            out = (jnp.dot(normed[at], weights, preferred_element_type=f32) + extra).astype(bf16)
            return [out[k * chunk : (k + 1) * chunk] for k in range(b - a)]

        half = n_ra // 2
        middle = share_of(half - 2, half + 2)
        part = share_of(0, half - 2) + middle + share_of(half + 2, n_ra)
        summed, before = ring_sum(part, rim)

        def scaled(x):
            total = jnp.sum(x[:, hid : hid + 2 * n_ra], axis=1, keepdims=True)
            return x * lax.rsqrt(total / model + EPS)

        lin, before = scaled(summed), scaled(before)
        positions = ((ra * chunk + jnp.arange(chunk, dtype=jnp.int32)) % LEN)[:, None]
        gate, up = (
            conv(lin[:, a : a + hid], before[:, a : a + hid], t[l].astype(f32), positions) + b[l].astype(f32)
            for a, t, b in ((0, gate_taps, gate_bias), (hid + pad, up_taps, up_bias))
        )
        hidden = (jax.nn.gelu(gate, approximate=True) * up).astype(bf16)
        down_rows = down_weight[l]
        partial = ring_apply(hidden, lambda h: jnp.dot(h, down_rows, preferred_element_type=f32).astype(bf16))
        partial = rolled(partial, (n_ra - ra + per * core) % n_ra, chunk)
        pair = (partial[:share].astype(f32) + other_core(partial[share:]).astype(f32)).astype(bf16)
        chips = [pair] + [along_chips(pair, k) for k in range(1, lax.axis_size("cb") // CORES)]
        branch = total_of([c.astype(f32) for c in chips])
        post_scale = lax.rsqrt(total_along_ra(jnp.sum(branch * branch, axis=1)) / model + EPS)[:, None]
        own = (RESIDUAL * widened[:share] + branch * post_scale * post_gain[l].astype(f32)).astype(bf16)
        state = jnp.concatenate([own, other_core(own)], axis=0)
    return rolled(state, core, share)


def solution(mesh):
    in_specs = (
        P("grp", "ra"),
        P(None, "ra"),
        P(None, "ra"),
        P(None, "ra", "cb"),
        P(None, "ra", "cb"),
        P(None, None, "cb"),
        P(None, None, "cb"),
        P(None, "cb"),
        P(None, "cb"),
        P(None, "cb", "ra"),
    )
    return jax.shard_map(local, mesh=mesh, in_specs=in_specs, out_specs=P("grp", "ra"), check_vma=False)
```

```python
import jax
import jax.numpy as jnp
from jax import lax
from jax.sharding import PartitionSpec as P

LEN = 256
LANES = 128
SUBLANES = 8
CORES = 2
EPS = 1e-06
RESIDUAL = 0.5

f32, bf16 = jnp.float32, jnp.bfloat16


def along_ra(x, by):
    n = lax.axis_size("ra")
    return lax.ppermute(x, "ra", [(i, (i + by) % n) for i in range(n)])


def along_chips(x, by):
    n = lax.axis_size("cb")
    return lax.ppermute(x, "cb", [(i, (i + CORES * by) % n) for i in range(n)])


def other_core(x):
    n = lax.axis_size("cb")
    return lax.ppermute(x, "cb", [(i, i ^ 1) for i in range(n)])


def rolled(x, by, unit):
    n = x.shape[0]
    return lax.dynamic_slice_in_dim(jnp.concatenate([x, x], axis=0), by * unit, n, 0)


def swapped(x, core):
    half = x.shape[0] // CORES
    return jnp.where(core == 1, jnp.concatenate([x[half:], x[:half]], axis=0), x)


def ring_sum(part, rim, beside):
    n = len(part)
    half = n // 2
    down, up = part[half], part[half - 1]
    for s in range(half - 1):
        got = along_ra(down, -1)
        down = (got.astype(f32) + part[half + 1 + s].astype(f32)).astype(bf16)
        if s == half - 4:
            down, beside = lax.optimization_barrier((down, beside))
        got = along_ra(up, 1)
        if s < half - 2:
            up = (got.astype(f32) + part[half - 2 - s].astype(f32)).astype(bf16)
        else:
            up = lax.optimization_barrier(got.astype(f32) + part[0].astype(f32))
    before = along_ra(up[-SUBLANES:].astype(bf16), 1)
    got = along_ra(down, -1)
    before = (before.astype(f32) + down[-SUBLANES:].astype(f32))[-rim:]
    return got.astype(f32) + up, before, beside


def ring_apply(own, apply):
    n = lax.axis_size("ra")
    half, rows = n // 2, own.shape[0]
    far = half // 2 + 1
    out = {0: apply(own)}
    held = {}
    for k in range(far - 1):
        fresh = []
        for sign in (1, -1):
            ends = [1 + k] + ([far + k] if far + k <= (half if sign > 0 else half - 1) else [])
            if k == 0:
                held[sign] = jnp.concatenate([along_ra(own, -sign * e) for e in ends], axis=0)
            else:
                held[sign] = along_ra(held[sign][: len(ends) * rows], -sign)
            fresh += [sign * e % n for e in ends]
        both = apply(jnp.concatenate([held[1], held[-1]], axis=0))
        for i, at in enumerate(fresh):
            out[at] = both[i * rows : (i + 1) * rows]
    return jnp.concatenate([out[at] for at in range(n)], axis=0)


def total_along_ra(x):
    n = lax.axis_size("ra")
    copies = jnp.broadcast_to(x, (n, 1, x.shape[0]))
    return jnp.sum(lax.all_to_all(copies, "ra", split_axis=0, concat_axis=0, tiled=True), axis=(0, 1))


def total_of(values):
    while len(values) > 1:
        half = len(values) // 2
        values = [values[k] + values[k + half] for k in range(half)]
    return values[0]


def conv(values, before, taps, positions):
    n, rows = taps.shape[0], values.shape[0]
    extended = jnp.concatenate([before, values], axis=0)
    result = taps[n - 1] * values
    for k in range(1, n):
        moved = extended[n - 1 - k : n - 1 - k + rows]
        result = result + taps[n - 1 - k] * jnp.where(positions >= k, moved, f32(0.0))
    return result


def local(
    tokens, pre_gain, post_gain, gate_weight, up_weight, gate_taps, up_taps, gate_bias, up_bias, down_weight
):
    n_ra = lax.axis_size("ra")
    ra, core = lax.axis_index("ra"), lax.axis_index("cb") % CORES
    layers, width = pre_gain.shape
    rows = tokens.shape[0]
    model = width * n_ra
    chunk, share = rows // n_ra, rows // CORES
    hid = gate_weight.shape[2]
    pad = -hid % LANES
    per = n_ra // CORES
    rim = gate_taps.shape[1] - 1

    def prepared(l):
        return jnp.concatenate([jnp.pad(w[l], ((0, 0), (0, pad))) for w in (gate_weight, up_weight)], axis=1)

    def layer(l, carried):
        state, weights = carried
        widened = state.astype(f32)
        squares = jnp.sum(widened * widened, axis=1, keepdims=True)
        normed = (widened * pre_gain[l].astype(f32)).astype(bf16)
        high = squares.astype(bf16).astype(f32)
        lane = lax.broadcasted_iota(jnp.int32, (1, 2 * (hid + pad)), 1) - hid
        to_own = (ra + per * core) % n_ra
        normed = rolled(normed, to_own, chunk)
        high, low = rolled(high, to_own, chunk), rolled(squares - high, to_own, chunk)

        def share_of(a, b):
            at = slice(a * chunk, b * chunk)
            extra = jnp.where(lane == ra, high[at], jnp.where(lane == n_ra + ra, low[at], f32(0.0)))
            out = (jnp.dot(normed[at], weights, preferred_element_type=f32) + extra).astype(bf16)
            return [out[k * chunk : (k + 1) * chunk] for k in range(b - a)]

        half = n_ra // 2
        middle = share_of(half - 2, half + 2)
        part = share_of(0, half - 2) + middle + share_of(half + 2, n_ra)
        summed, before, following = ring_sum(part, rim, prepared((l + 1) % layers))

        def scaled(x):
            total = jnp.sum(x[:, hid : hid + 2 * n_ra], axis=1, keepdims=True)
            return x * lax.rsqrt(total / model + EPS)

        lin, before = scaled(summed), scaled(before)
        positions = ((ra * chunk + jnp.arange(chunk, dtype=jnp.int32)) % LEN)[:, None]
        gate, up = (
            conv(lin[:, a : a + hid], before[:, a : a + hid], t[l].astype(f32), positions) + b[l].astype(f32)
            for a, t, b in ((0, gate_taps, gate_bias), (hid + pad, up_taps, up_bias))
        )
        hidden = (jax.nn.gelu(gate, approximate=True) * up).astype(bf16)
        down_rows = down_weight[l]
        partial = ring_apply(hidden, lambda h: jnp.dot(h, down_rows, preferred_element_type=f32).astype(bf16))
        partial = rolled(partial, (n_ra - ra + per * core) % n_ra, chunk)
        pair = (partial[:share].astype(f32) + other_core(partial[share:]).astype(f32)).astype(bf16)
        chips = [pair] + [along_chips(pair, k) for k in range(1, lax.axis_size("cb") // CORES)]
        branch = total_of([c.astype(f32) for c in chips])
        post_scale = lax.rsqrt(total_along_ra(jnp.sum(branch * branch, axis=1)) / model + EPS)[:, None]
        own = (RESIDUAL * widened[:share] + branch * post_scale * post_gain[l].astype(f32)).astype(bf16)
        return jnp.concatenate([own, other_core(own)], axis=0), following

    state, _ = lax.fori_loop(0, layers, layer, (swapped(tokens, core), prepared(0)))
    return swapped(state, core)


def solution(mesh):
    in_specs = (
        P("grp", "ra"),
        P(None, "ra"),
        P(None, "ra"),
        P(None, "ra", "cb"),
        P(None, "ra", "cb"),
        P(None, None, "cb"),
        P(None, None, "cb"),
        P(None, "cb"),
        P(None, "cb"),
        P(None, "cb", "ra"),
    )
    return jax.shard_map(local, mesh=mesh, in_specs=in_specs, out_specs=P("grp", "ra"), check_vma=False)
```
